256 devices in a mesh: fs: 32 (over z, y), tp: 8 (over x, core).
Axes of the slice: x: 4, y: 4, z: 8, core: 2. Of those that a mesh axis runs over, the one named last changes fastest.
Arguments:
- prompt: bfloat16 [24576, 2048], P('fs'), may hold values from -6 to 6
- routes: int32 [24576, 2], P('fs'), may hold values from 0 to 63, all different within a row; in each aligned block of 768 rows (0 to 767, 768 to 1535, ...) at most 48 rows name the same one
- affinity: float32 [24576, 2], P('fs'), may hold values from 0.05 to 1
- norm_gain: float32 [2048], P('fs'), may hold values from 0.1 to 1.9
- gate_master: float32 [64, 2048, 1024], P(None, 'fs', 'tp'), may hold values from -0.125 to 0.125
- up_master: float32 [64, 2048, 1024], P(None, 'fs', 'tp'), may hold values from -0.125 to 0.125
- down_master: float32 [64, 1024, 2048], P(None, 'fs', 'tp'), may hold values from -0.1875 to 0.1875
Outputs:
- mixed: bfloat16 [24576, 2048], P('fs', 'tp')
- gate_weights: bfloat16 [64, 2048, 1024], P('fs', None, 'tp')
- up_weights: bfloat16 [64, 2048, 1024], P('fs', None, 'tp')
- down_weights: bfloat16 [64, 1024, 2048], P('fs', None, 'tp')
The draws below stay inside these ranges and needn't reach their ends.
Inputs may be any that keep to these rules, and one draw needn't show every extreme that they name: `routes`: each row names 2 different experts. In each aligned block of 768 rows no expert is named more than 48 times, a bound that some block reaches.
All inputs are finite; a program needn't handle non-finite values.
Results may differ from the reference program's by a relative error of at most 0.0086.
Values may be sent and summed in bfloat16 or wider, within the bound.
No kernel may reach another device: no remote copies, remote signals or barrier semaphores. Data moves between devices by JAX's collectives and lax.ppermute only.
A program may use at most 128 MiB of HBM per device.

```python
import math
import jax
import jax.numpy as jnp
import numpy as np
from jax import lax

D = 2048
FF = 1024
TOP = 2
TOK_DEV = 768
EXPERTS = 64
TOKENS = 24576
CAP = 48
N_FS = 32


def block_levels(key, extent, split, smallest, top_value):
    def one(position, parts):
        draws = jax.random.uniform(jax.random.fold_in(jax.random.fold_in(key, 6), position), (parts,), jnp.float32, smallest / len(split), top_value / len(split))
        return jnp.repeat(jnp.exp(draws), extent[position] // parts).reshape((-1,) + (1,) * (len(extent) - position - 1))

    level = one(*split[0])
    for cut in split[1:]:
        level = level * one(*cut)
    return level


def assign_block(key, own, number, rows, amount, top, most, slope):
    ranking = jax.random.permutation(key, amount)
    crowded, common = shares(amount, rows * top, most, slope, True), shares(amount, rows * top, most, slope, False)
    places = jnp.arange(amount)

    def named(lengths, turn):
        used = int((lengths > 0).sum())
        fixed = max(1, used // 4)
        moved = fixed + (places - fixed + turn * (used - fixed)) % max(1, amount - fixed)
        return jnp.zeros((amount,), jnp.int32).at[ranking[jnp.where(places < fixed, places, moved)]].set(jnp.asarray(lengths, jnp.int32))

    lengths = jnp.where(number % 4 == 0, named(crowded, number // 4), named(common, number - number // 4 - 1))
    mixed = jax.random.permutation(jax.random.fold_in(own, 3), amount)
    source_of, taker = mixed[0:amount // 2 * 2:2], mixed[1:amount // 2 * 2:2]
    margin = jnp.minimum(lengths[source_of] - 1, most - lengths[taker]) // 2
    margin = jnp.where((source_of == ranking[0]) | (taker == ranking[0]) | (lengths[taker] == 0), 0, jnp.maximum(margin, 0))
    moved = jax.random.randint(jax.random.fold_in(own, 4), (amount // 2,), 0, 1 << 20) % (margin + 1)
    lengths = lengths.at[source_of].add(-moved).at[taker].add(moved)
    labels = jnp.searchsorted(jnp.cumsum(lengths), jnp.arange(rows * top), side="right").astype(jnp.int32)
    grid = labels.reshape(top, rows).T
    grid = grid[jax.random.permutation(jax.random.fold_in(own, 1), rows)]
    turn = jax.random.randint(jax.random.fold_in(own, 2), (rows, 1), 0, top)
    return jnp.take_along_axis(grid, (jnp.arange(top)[None, :] + turn) % top, axis=1)


def shares(count, total, bound, slope, full):
    weights = [(1 << 20) // math.isqrt(rank ** slope) + 1 for rank in range(1, count + 1)]
    largest = bound if full else min(bound, max(-(-total // count), total * weights[0] // sum(weights)))
    least = 1 if total - largest >= count - 1 else 0
    counts, rest = [largest] + [least] * (count - 1), total - largest - least * (count - 1)
    while rest > 0:
        free = [i for i in range(1, count) if counts[i] < largest] or [i for i in range(1, count) if counts[i] < bound]
        whole, left = sum([weights[i] for i in free]), rest
        for i in free:
            extra = min(bound - counts[i], max(1, left * weights[i] // whole), rest)
            counts[i] = counts[i] + extra
            rest = rest - extra
    return np.array(counts)


def noise(rng, dims, width, most, pieces=(), kind=jnp.bfloat16):
    gain = block_levels(rng, dims, pieces, -0.22, 0.18) if pieces else 1.0
    drawn = jax.random.normal(rng, dims, jnp.float32) * width * gain
    return jnp.minimum(jnp.maximum(drawn, -most), most).astype(kind)


def setup_inputs(seed: int = 0) -> dict:
    arg_keys = jax.random.split(jax.random.key(seed), 8)
    prompt = noise(arg_keys[0], (TOKENS, D), 1.0, 6.0, ((0, 32),))
    routes_keys = jax.random.split(jax.random.fold_in(arg_keys[1], 1), TOKENS // TOK_DEV)
    routes_turns = jax.random.permutation(jax.random.fold_in(arg_keys[1], 3), TOKENS // TOK_DEV)
    routes = jax.vmap(lambda own, number: assign_block(jax.random.fold_in(arg_keys[1], 2), own, number, TOK_DEV, EXPERTS, TOP, CAP, 2))(routes_keys, routes_turns).reshape((TOKENS, TOP))
    affinity = jnp.clip(0.05 + 0.95 * jax.random.uniform(arg_keys[2], (TOKENS, TOP), jnp.float32) ** block_levels(arg_keys[2], (TOKENS, TOP), ((0, 32),), -0.2, 0.2), 0.05, 1.0)
    norm_gain = jnp.clip(1.0 + 0.18 * jax.random.normal(arg_keys[3], (D,), jnp.float32), 0.1, 1.9)
    gate_master = noise(arg_keys[4], (EXPERTS, D, FF), D ** -0.5, 0.125, ((1, 32), (2, 8)), jnp.float32)
    up_master = noise(arg_keys[5], (EXPERTS, D, FF), D ** -0.5, 0.125, ((1, 32), (2, 8)), jnp.float32)
    down_master = noise(arg_keys[6], (EXPERTS, FF, D), FF ** -0.5, 0.1875, ((1, 32), (2, 8)), jnp.float32)
    return {"prompt": prompt, "routes": routes, "affinity": affinity, "norm_gain": norm_gain, "gate_master": gate_master, "up_master": up_master, "down_master": down_master}


norm_eps = 1e-06

def one_expert(operands):
    slot_rows, gate_weight, up_weight, down_weight = operands
    gate_pre = jnp.dot(slot_rows, gate_weight, preferred_element_type=jnp.float32)
    up_pre = jnp.dot(slot_rows, up_weight, preferred_element_type=jnp.float32)
    hidden = (jax.nn.silu(gate_pre) * up_pre).astype(jnp.bfloat16)
    return jnp.dot(hidden, down_weight, preferred_element_type=jnp.float32).astype(jnp.bfloat16)

def reference(prompt, routes, affinity, norm_gain, gate_master, up_master, down_master):
    gain_rows = norm_gain[None, :, None]
    gate_weights = (gate_master * gain_rows).astype(jnp.bfloat16)
    up_weights = (up_master * gain_rows).astype(jnp.bfloat16)
    down_weights = down_master.astype(jnp.bfloat16)
    values = prompt.astype(jnp.float32)
    normed = (values * lax.rsqrt(lax.optimization_barrier(jnp.mean(values * values, axis=-1, keepdims=True)) + norm_eps)).astype(jnp.bfloat16)
    flat_ids = routes.reshape(N_FS, TOK_DEV * TOP)
    onehot = (flat_ids[:, :, None] == jnp.arange(EXPERTS, dtype=jnp.int32)[None, None, :]).astype(jnp.int32)
    slot_rank = lax.optimization_barrier(jnp.sum(jnp.cumsum(onehot, axis=1) * onehot, axis=2)) - 1
    column = (jnp.arange(N_FS, dtype=jnp.int32)[:, None] * CAP + slot_rank).reshape(-1).astype(jnp.int32)
    expert_of = flat_ids.reshape(-1).astype(jnp.int32)
    token_of = (jnp.arange(TOKENS * TOP, dtype=jnp.int32) // TOP).astype(jnp.int32)
    buffer = jnp.zeros((EXPERTS, N_FS * CAP, D), jnp.bfloat16).at[expert_of, column].set(normed[token_of])
    outputs = lax.map(one_expert, (buffer, gate_weights, up_weights, down_weights))
    picked = outputs[expert_of, column].reshape(TOKENS, TOP, D).astype(jnp.float32)
    share = affinity / lax.optimization_barrier(jnp.sum(affinity, axis=1, keepdims=True))
    mixed = lax.optimization_barrier(jnp.sum(share[:, :, None] * picked, axis=1)).astype(jnp.bfloat16)
    return (mixed, gate_weights, up_weights, down_weights)
```

```python
import functools
import jax
import jax.numpy as jnp
from jax import lax
from jax.experimental import pallas as pl
from jax.experimental.pallas import tpu as pltpu
from jax.sharding import PartitionSpec as P

norm_eps = 1e-06
VMEM_LIMIT = 48 * 1024 * 1024


def dispatch_kernel(row_steps, cap, experts, tp_ref, routes_ref, prompt_ref, out_ref, slots_ref, normed_ref):
    step = pl.program_id(0)
    tokens = routes_ref.shape[1]
    width = normed_ref.shape[1]
    rows = prompt_ref.shape[0]

    @pl.when(step == 0)
    def _():
        ids = routes_ref[...]
        expert = lax.broadcasted_iota(jnp.int32, (experts, tokens), 0)
        hit0 = ids[0:1, :] == expert
        hit1 = ids[1:2, :] == expert
        named = jnp.where(hit0 | hit1, 1.0, 0.0).astype(jnp.bfloat16)
        earlier = lax.broadcasted_iota(jnp.int32, (tokens, tokens), 0) < lax.broadcasted_iota(
            jnp.int32, (tokens, tokens), 1
        )
        before = jnp.where(earlier, 1.0, 0.0).astype(jnp.bfloat16)
        count = jnp.dot(named, before, preferred_element_type=jnp.float32)
        rank0 = jnp.sum(jnp.where(hit0, count, 0.0), axis=0, keepdims=True).astype(jnp.int32)
        rank1 = jnp.sum(jnp.where(hit1, count, 0.0), axis=0, keepdims=True).astype(jnp.int32)
        slots_ref[0:1, :] = ids[0:1, :] * cap + rank0
        slots_ref[1:2, :] = ids[1:2, :] * cap + rank1

    @pl.when(step < row_steps)
    def _():
        values = prompt_ref[...].astype(jnp.float32)
        scale = lax.rsqrt(jnp.mean(values * values, axis=1, keepdims=True) + norm_eps)
        start = pl.multiple_of(tp_ref[0] * width, width)
        part = prompt_ref[:, pl.ds(start, width)].astype(jnp.float32)
        normed_ref[pl.ds(pl.multiple_of(step * rows, rows), rows), :] = (part * scale).astype(jnp.bfloat16)

    @pl.when(step >= row_steps)
    def _():
        block = out_ref.shape[0]
        slot = lax.broadcasted_iota(jnp.int32, (block, tokens), 0) + (step - row_steps) * block
        chosen = (slots_ref[0:1, :] == slot) | (slots_ref[1:2, :] == slot)
        out_ref[...] = jnp.dot(
            jnp.where(chosen, 1.0, 0.0).astype(jnp.bfloat16),
            normed_ref[...],
            preferred_element_type=jnp.float32,
        ).astype(jnp.bfloat16)


def dispatch(prompt, routes, tp_index, cap, experts, width):
    tokens, model_width = prompt.shape
    row_steps, slot_steps = 4, 4
    rows, block = tokens // row_steps, experts * cap // slot_steps
    return pl.pallas_call(
        functools.partial(dispatch_kernel, row_steps, cap, experts),
        grid_spec=pltpu.PrefetchScalarGridSpec(
            num_scalar_prefetch=1,
            grid=(row_steps + slot_steps,),
            in_specs=[
                pl.BlockSpec((2, tokens), lambda i, tp: (0, 0)),
                pl.BlockSpec((rows, model_width), lambda i, tp: (jnp.minimum(i, row_steps - 1), 0)),
            ],
            out_specs=[
                pl.BlockSpec((block, width), lambda i, tp: (jnp.maximum(i - row_steps, 0), 0)),
                pl.BlockSpec((2, tokens), lambda i, tp: (0, 0)),
            ],
            scratch_shapes=[pltpu.VMEM((tokens, width), jnp.bfloat16)],
        ),
        out_shape=[
            jax.ShapeDtypeStruct((experts * cap, width), jnp.bfloat16),
            jax.ShapeDtypeStruct((2, tokens), jnp.int32),
        ],
        compiler_params=pltpu.CompilerParams(
            dimension_semantics=("arbitrary",), vmem_limit_bytes=VMEM_LIMIT
        ),
        name="dispatch",
    )(tp_index, routes.T, prompt)


def combine_kernel(slots_ref, affinity_ref, rows_ref, out_ref, first_ref, second_ref):
    step = pl.program_id(0)
    tokens = slots_ref.shape[0]
    block = rows_ref.shape[0]
    slot = lax.broadcasted_iota(jnp.int32, (tokens, block), 1) + step * block
    rows = rows_ref[...]

    @pl.when(step == 0)
    def _():
        first_ref[...] = jnp.zeros_like(first_ref)
        second_ref[...] = jnp.zeros_like(second_ref)

    for k, total in ((0, first_ref), (1, second_ref)):
        chosen = jnp.where(slots_ref[:, k : k + 1] == slot, 1.0, 0.0).astype(jnp.bfloat16)
        total[...] += jnp.dot(chosen, rows, preferred_element_type=jnp.float32)

    @pl.when(step == pl.num_programs(0) - 1)
    def _():
        affinity = affinity_ref[...]
        share = affinity / jnp.sum(affinity, axis=1, keepdims=True)
        out_ref[...] = (share[:, 0:1] * first_ref[...] + share[:, 1:2] * second_ref[...]).astype(jnp.bfloat16)


def combine(slots, affinity, rows):
    tokens = affinity.shape[0]
    slot_count, width = rows.shape
    steps = 4
    block = slot_count // steps
    return pl.pallas_call(
        combine_kernel,
        grid=(steps,),
        in_specs=[
            pl.BlockSpec((tokens, 2), lambda i: (0, 0)),
            pl.BlockSpec((tokens, 2), lambda i: (0, 0)),
            pl.BlockSpec((block, width), lambda i: (i, 0)),
        ],
        out_specs=pl.BlockSpec((tokens, width), lambda i: (0, 0)),
        scratch_shapes=[pltpu.VMEM((tokens, width), jnp.float32)] * 2,
        out_shape=jax.ShapeDtypeStruct((tokens, width), jnp.bfloat16),
        compiler_params=pltpu.CompilerParams(
            dimension_semantics=("arbitrary",), vmem_limit_bytes=VMEM_LIMIT
        ),
        name="combine",
    )(slots.T, affinity, rows)


WHOLE = ((0, 0), (0, 1), (3, 0), (3, 1), (1, 0), (1, 1))
SPLIT = ((2, 0), (2, 1))


def expert_matmul_kernel(gated, half_step, tp_ref, *refs):
    whole, low, high = refs[:6], refs[6:8], refs[8:10]
    weight_ref, out_ref, total_ref = refs[10:]
    sources, _, cap, width = whole[0].shape
    rows = sources * cap
    group = weight_ref.shape[0] // 8
    step = pl.program_id(1)

    index = tp_ref[0]

    def product(piece, position):
        dx, swap = (WHOLE + SPLIT)[position]
        source = (((index >> 1) + dx) & 3) * 2 + ((index & 1) ^ swap)
        block = weight_ref[pl.ds(source * group, group), 0]
        return jnp.dot(
            piece[:, 0].reshape(rows, width),
            block.reshape(width, block.shape[-1]),
            preferred_element_type=jnp.float32,
        )

    total = product(whole[0], 0)
    for position in range(1, 6):
        total += product(whole[position], position)
    total_ref[...] = total

    @pl.when(step < half_step)
    def _():
        total_ref[...] += product(low[0], 6) + product(low[1], 7)

    @pl.when(step >= half_step)
    def _():
        total_ref[...] += product(high[0], 6) + product(high[1], 7)

    result = total_ref[...]
    if gated:
        half = result.shape[1] // 2
        gate, up = result[:, :half], result[:, half:]
        result = gate / (1.0 + jnp.exp(-gate)) * up
    out_ref[...] = result.astype(jnp.bfloat16).reshape(out_ref.shape)


def expert_matmul(pieces, weight, order, gated, out_width):
    whole, low, high = pieces
    sources, experts, cap, width = whole[0].shape
    steps = 4
    chunk = sources // steps
    half_step = steps // 2
    block = (chunk, 1, cap, width)
    rows = chunk * cap
    return pl.pallas_call(
        functools.partial(expert_matmul_kernel, gated, half_step),
        grid_spec=pltpu.PrefetchScalarGridSpec(
            num_scalar_prefetch=1,
            grid=(experts, steps),
            in_specs=[pl.BlockSpec(block, lambda e, j, o: (j, e, 0, 0))] * 6
            + [pl.BlockSpec(block, lambda e, j, o: (jnp.minimum(j, half_step - 1), e, 0, 0))] * 2
            + [pl.BlockSpec(block, lambda e, j, o: (jnp.maximum(j - half_step, 0), e, 0, 0))] * 2
            + [pl.BlockSpec((sources, 1) + weight.shape[2:], lambda e, j, o: (0, e, 0, 0))],
            out_specs=pl.BlockSpec((chunk, 1, cap, out_width), lambda e, j, o: (j, e, 0, 0)),
            scratch_shapes=[pltpu.VMEM((rows, weight.shape[-1]), jnp.float32)],
        ),
        out_shape=jax.ShapeDtypeStruct((sources, experts, cap, out_width), jnp.bfloat16),
        compiler_params=pltpu.CompilerParams(
            dimension_semantics=("arbitrary", "arbitrary"), vmem_limit_bytes=VMEM_LIMIT
        ),
    )(order, *whole, *low, *high, weight)


def tp_move(dx, swap):
    return [(2 * x + c, 2 * ((x + dx) % 4) + (c ^ swap)) for x in range(4) for c in range(2)]


def spread(own):
    half = own.shape[0] // 2
    right = lax.ppermute(own, "tp", tp_move(1, 0))
    left = lax.ppermute(own, "tp", tp_move(3, 0))
    own_other = lax.ppermute(own, "tp", tp_move(0, 1))
    low = lax.ppermute(right[:half], "tp", tp_move(1, 0))
    high = lax.ppermute(left[half:], "tp", tp_move(3, 0))
    right_other = lax.ppermute(right, "tp", tp_move(0, 1))
    left_other = lax.ppermute(left, "tp", tp_move(0, 1))
    low_other = lax.ppermute(low, "tp", tp_move(0, 1))
    high_other = lax.ppermute(high, "tp", tp_move(0, 1))
    return (own, own_other, right, right_other, left, left_other), (low, low_other), (high, high_other)


def exchange(array):
    return lax.all_to_all(array, "fs", split_axis=0, concat_axis=0, tiled=True)


def layer(prompt, routes, affinity, norm_gain, gate_master, up_master, down_master):
    fs_count, tp_count = lax.axis_size("fs"), lax.axis_size("tp")
    experts, gain_rows, hidden_width = gate_master.shape
    here = experts // fs_count
    token_count, top_count = routes.shape
    capacity = 2 * token_count * top_count // experts
    width = prompt.shape[1] // tp_count
    tp_index = lax.axis_index("tp").astype(jnp.int32)
    tp_index = tp_index.reshape(1)

    outbox, slots = dispatch(prompt, routes, tp_index, capacity, experts, width)
    received = exchange(outbox.reshape(fs_count, here, capacity, width))

    gain = norm_gain[None, :, None]
    gate_up = jnp.concatenate(
        [(gate_master * gain).astype(jnp.bfloat16), (up_master * gain).astype(jnp.bfloat16)], axis=2
    ).reshape(fs_count, here, gain_rows, 2 * hidden_width)
    down = down_master.astype(jnp.bfloat16).reshape((fs_count, here) + down_master.shape[1:])

    pieces = spread(received)
    gate_up_new = exchange(gate_up)
    hidden = expert_matmul(pieces, gate_up_new, tp_index, True, hidden_width)
    down_new = exchange(down)
    expert_out = expert_matmul(spread(hidden), down_new, tp_index, False, width)
    returned = exchange(expert_out)
    mixed = combine(slots, affinity, returned.reshape(experts * capacity, width))

    def rows_first(array):
        return array.transpose(1, 0, 2, 3).reshape(here, -1, array.shape[-1])

    return (
        mixed,
        rows_first(gate_up_new[..., :hidden_width]),
        rows_first(gate_up_new[..., hidden_width:]),
        rows_first(down_new),
    )


def solution(mesh):
    in_specs = (
        P("fs", None),
        P("fs", None),
        P("fs", None),
        P("fs"),
        P(None, "fs", "tp"),
        P(None, "fs", "tp"),
        P(None, "fs", "tp"),
    )
    out_specs = (P("fs", "tp"), P("fs", None, "tp"), P("fs", None, "tp"), P("fs", None, "tp"))
    return jax.shard_map(layer, mesh=mesh, in_specs=in_specs, out_specs=out_specs, check_vma=False)
```

```python
import functools
import jax
import jax.numpy as jnp
from jax import lax
from jax.experimental import pallas as pl
from jax.experimental.pallas import tpu as pltpu
from jax.sharding import PartitionSpec as P

norm_eps = 1e-06
MIB = 1024 * 1024


def dispatch_kernel(cap, tp_ref, routes_ref, prompt_ref, out_ref, slots_ref, held, normed, key, choice, outbox, in_sem, out_sem):
    parts, rows, _ = held.shape
    experts, tokens = key.shape
    width = normed.shape[1]
    block = outbox.shape[1]
    loads = [
        pltpu.make_async_copy(prompt_ref.at[pl.ds(k * rows, rows)], held.at[k], in_sem.at[k])
        for k in range(parts)
    ]
    for load in loads:
        load.start()

    ids = routes_ref[...]
    expert = lax.broadcasted_iota(jnp.int32, (experts, tokens), 0)
    hit0 = ids[0:1, :] == expert
    hit1 = ids[1:2, :] == expert
    named = hit0 | hit1
    earlier = lax.broadcasted_iota(jnp.int32, (tokens, tokens), 0) < lax.broadcasted_iota(
        jnp.int32, (tokens, tokens), 1
    )
    count = jnp.dot(
        jnp.where(named, 1.0, 0.0).astype(jnp.bfloat16),
        jnp.where(earlier, 1.0, 0.0).astype(jnp.bfloat16),
        preferred_element_type=jnp.float32,
    )
    key[...] = jnp.where(named, count, -1.0).astype(jnp.int32)
    rank0 = jnp.sum(jnp.where(hit0, count, 0.0), axis=0, keepdims=True).astype(jnp.int32)
    rank1 = jnp.sum(jnp.where(hit1, count, 0.0), axis=0, keepdims=True).astype(jnp.int32)
    slots_ref[0:1, :] = ids[0:1, :] * cap + rank0
    slots_ref[1:2, :] = ids[1:2, :] * cap + rank1

    def fill(group, _):
        rank = lax.broadcasted_iota(jnp.int32, (cap, tokens), 0)
        first = pl.multiple_of(group * 8, 8)
        keys = key[pl.ds(first, 8), :]
        for k in range(8):
            choice[pl.ds(pl.multiple_of((first + k) * cap, cap), cap), :] = jnp.where(
                keys[k : k + 1, :] == rank, 1.0, 0.0
            ).astype(jnp.bfloat16)
        return 0

    lax.fori_loop(0, experts // 8, fill, 0)

    start = pl.multiple_of(tp_ref[0] * width, width)
    for k in range(parts):
        loads[k].wait()
        values = held[k].astype(jnp.float32)
        scale = lax.rsqrt(jnp.mean(values * values, axis=1, keepdims=True) + norm_eps)
        part = held[k, :, pl.ds(start, width)].astype(jnp.float32)
        normed[pl.ds(k * rows, rows), :] = (part * scale).astype(jnp.bfloat16)

    stores = []
    for k in range(outbox.shape[0]):
        outbox[k] = jnp.dot(
            choice[pl.ds(k * block, block), :], normed[...], preferred_element_type=jnp.float32
        ).astype(jnp.bfloat16)
        stores.append(
            pltpu.make_async_copy(outbox.at[k], out_ref.at[pl.ds(k * block, block)], out_sem.at[k])
        )
        stores[k].start()
    for store in stores:
        store.wait()


def dispatch(prompt, routes, tp_index, cap, experts, width):
    tokens, model_width = prompt.shape
    parts = 4
    rows, block = tokens // parts, experts * cap // parts
    return pl.pallas_call(
        functools.partial(dispatch_kernel, cap),
        in_specs=[
            pl.BlockSpec(memory_space=pltpu.SMEM),
            pl.BlockSpec(memory_space=pltpu.VMEM),
            pl.BlockSpec(memory_space=pltpu.HBM),
        ],
        out_specs=[
            pl.BlockSpec(memory_space=pltpu.HBM),
            pl.BlockSpec(memory_space=pltpu.VMEM),
        ],
        scratch_shapes=[
            pltpu.VMEM((parts, rows, model_width), jnp.bfloat16),
            pltpu.VMEM((tokens, width), jnp.bfloat16),
            pltpu.VMEM((experts, tokens), jnp.int32),
            pltpu.VMEM((experts * cap, tokens), jnp.bfloat16),
            pltpu.VMEM((parts, block, width), jnp.bfloat16),
            pltpu.SemaphoreType.DMA((parts,)),
            pltpu.SemaphoreType.DMA((parts,)),
        ],
        out_shape=[
            pltpu.HBM((experts * cap, width), jnp.bfloat16),
            jax.ShapeDtypeStruct((2, tokens), jnp.int32),
        ],
        compiler_params=pltpu.CompilerParams(vmem_limit_bytes=48 * MIB),
        name="dispatch",
    )(tp_index, routes.T, pltpu.with_memory_space_constraint(prompt, pltpu.HBM))


def combine_kernel(slots_ref, share_ref, rows_ref, out_ref):
    tokens = slots_ref.shape[1]
    block = rows_ref.shape[0] // 12
    share = share_ref[...]
    total = None
    for k in range(12):
        slot = lax.broadcasted_iota(jnp.int32, (block, tokens), 0) + k * block
        second = jnp.where(slots_ref[1:2, :] == slot, share[1:2, :], 0.0)
        weights = jnp.where(slots_ref[0:1, :] == slot, share[0:1, :], second).astype(jnp.bfloat16)
        product = lax.dot_general(
            weights,
            rows_ref[pl.ds(k * block, block), :],
            (((0,), (0,)), ((), ())),
            preferred_element_type=jnp.float32,
        )
        total = product if total is None else total + product
    out_ref[...] = total.astype(jnp.bfloat16)


def combine(slots, share, rows):
    whole = pl.BlockSpec(memory_space=pltpu.VMEM)
    return pl.pallas_call(
        combine_kernel,
        in_specs=[whole] * 3,
        out_specs=whole,
        out_shape=jax.ShapeDtypeStruct((slots.shape[1], rows.shape[1]), jnp.bfloat16),
        compiler_params=pltpu.CompilerParams(vmem_limit_bytes=48 * MIB),
        name="combine",
    )(slots, share, rows)


PLACES = ((0, 0), (0, 1), (3, 0), (3, 1), (1, 0), (1, 1), (2, 0), (2, 1))


def expert_matmul_kernel(gated, blocks, begin, out_begin, tp_ref, *refs):
    pieces, weight_ref, out_ref = refs[:8], refs[8], refs[-7]
    held, matrices, result, piece_sem, weight_sem, out_sem = refs[-6:]
    experts, count, cap, _ = held.shape
    width = pieces[0].shape[-1]
    group = matrices.shape[1] // 8
    index = tp_ref[0]

    loads = []
    for e in range(experts):
        for p in range(8):
            dx, swap = PLACES[p]
            source = (((index >> 1) + dx) & 3) * 2 + ((index & 1) ^ swap)
            first = begin if pieces[p].shape[0] > count else 0
            loads.append(
                pltpu.make_async_copy(
                    weight_ref.at[pl.ds(source * group, group), e],
                    matrices.at[e, pl.ds(p * group, group)],
                    weight_sem.at[e, p],
                )
            )
            loads.append(
                pltpu.make_async_copy(
                    pieces[p].at[pl.ds(first, count), e],
                    held.at[e, :, :, pl.ds(p * width, width)],
                    piece_sem.at[e, p],
                )
            )
    for load in loads:
        load.start()

    stores = []
    part = count // blocks
    for e in range(experts):
        for load in loads[16 * e : 16 * e + 16]:
            load.wait()
        right = matrices[e].reshape(8 * width, matrices.shape[-1])
        for b in range(blocks):
            span = pl.ds(b * part, part)
            left = held[e, span].reshape(part * cap, 8 * width)
            total = jnp.dot(left, right, preferred_element_type=jnp.float32)
            if gated:
                half = total.shape[1] // 2
                gate, up = total[:, :half], total[:, half:]
                total = gate / (1.0 + jnp.exp(-gate)) * up
            result[e, span] = total.astype(jnp.bfloat16).reshape((part,) + result.shape[2:])
        stores.append(
            pltpu.make_async_copy(
                result.at[e], out_ref.at[pl.ds(out_begin, count), e], out_sem.at[e]
            )
        )
        stores[e].start()
    for store in stores:
        store.wait()


def expert_matmul(pieces, weight, tp_index, half, gated, blocks, into):
    cap, width = pieces[0].shape[-2:]
    sources, experts = weight.shape[0], weight.shape[1]
    out_width = weight.shape[-1] // 2 if gated else weight.shape[-1]
    count = sources // 2
    anywhere = pl.BlockSpec(memory_space=pl.ANY)
    operands = [*pieces, weight]
    aliases = {}
    if into is not None:
        operands.append(into)
        aliases = {len(operands): 0}
    out_shape = pltpu.HBM((count if gated else sources, experts, cap, out_width), jnp.bfloat16)
    operands = [pltpu.with_memory_space_constraint(array, pltpu.HBM) for array in operands]
    return pl.pallas_call(
        functools.partial(
            expert_matmul_kernel, gated, blocks, half * count, 0 if gated else half * count
        ),
        in_specs=[pl.BlockSpec(memory_space=pltpu.SMEM)] + [anywhere] * len(operands),
        out_specs=pl.BlockSpec(memory_space=pltpu.HBM),
        out_shape=out_shape,
        scratch_shapes=[
            pltpu.VMEM((experts, count, cap, 8 * width), jnp.bfloat16),
            pltpu.VMEM((experts, sources) + weight.shape[2:], jnp.bfloat16),
            pltpu.VMEM((experts, count, cap, out_width), jnp.bfloat16),
            pltpu.SemaphoreType.DMA((experts, 8)),
            pltpu.SemaphoreType.DMA((experts, 8)),
            pltpu.SemaphoreType.DMA((experts,)),
        ],
        input_output_aliases=aliases,
        compiler_params=pltpu.CompilerParams(vmem_limit_bytes=48 * MIB),
    )(tp_index, *operands)


def tp_move(dx, swap):
    return [(2 * x + c, 2 * ((x + dx) % 4) + (c ^ swap)) for x in range(4) for c in range(2)]


def move(array, dx, swap):
    return lax.ppermute(array, "tp", tp_move(dx, swap))


def spread_tokens(own):
    half = own.shape[0] // 2
    first, second = own[:half], own[half:]
    right_first = move(first, 1, 0)
    left_second = move(second, 3, 0)
    right_second = move(second, 1, 0)
    left_first = move(first, 3, 0)
    own_other = move(own, 0, 1)
    far_first = move(right_first, 1, 0)
    far_second = move(left_second, 3, 0)

    def both(piece):
        return piece, move(piece, 0, 1)

    return (
        (own, own_other)
        + both(right_first)
        + both(left_first)
        + both(far_first),
        (own, own_other)
        + both(right_second)
        + both(left_second)
        + both(far_second),
    )


def spread_hidden(own, half):
    right = move(own, 1, 0)
    left = move(own, 3, 0)
    far = move(right, 1, 0) if half == 0 else move(left, 3, 0)
    own_other = move(own, 0, 1)
    right_other = move(right, 0, 1)
    left_other = move(left, 0, 1)
    far_other = move(far, 0, 1)
    return own, own_other, right, right_other, left, left_other, far, far_other


def exchange(array):
    return lax.all_to_all(array, "fs", split_axis=0, concat_axis=0, tiled=True)


def layer(prompt, routes, affinity, norm_gain, gate_master, up_master, down_master):
    fs_count, tp_count = lax.axis_size("fs"), lax.axis_size("tp")
    experts, gain_rows, hidden_width = gate_master.shape
    here = experts // fs_count
    token_count, top_count = routes.shape
    capacity = 2 * token_count * top_count // experts
    width = prompt.shape[1] // tp_count
    tp_index = lax.axis_index("tp").astype(jnp.int32)
    tp_index = tp_index.reshape(1)

    outbox, slots = dispatch(prompt, routes, tp_index, capacity, experts, width)
    received = exchange(outbox.reshape(fs_count, here, capacity, width))

    gain = norm_gain[None, :, None]
    gate_up = jnp.concatenate(
        [(gate_master * gain).astype(jnp.bfloat16), (up_master * gain).astype(jnp.bfloat16)], axis=2
    ).reshape(fs_count, here, gain_rows, 2 * hidden_width)
    pieces = spread_tokens(received)
    swapped = [piece for half in pieces for piece in half[1::2]]
    affinity = lax.optimization_barrier((affinity, *swapped))[0].T
    share = affinity / jnp.sum(affinity, axis=0, keepdims=True)
    down = down_master.astype(jnp.bfloat16).reshape((fs_count, here) + down_master.shape[1:])
    gate_up_new = exchange(gate_up)
    down_new = exchange(down)
    hidden = [
        spread_hidden(expert_matmul(pieces[half], gate_up_new, tp_index, half, True, 2, None), half)
        for half in range(2)
    ]
    expert_out = None
    for half in range(2):
        expert_out = expert_matmul(hidden[half], down_new, tp_index, half, False, 2, expert_out)
    returned = exchange(expert_out)
    mixed = combine(slots, share, returned.reshape(experts * capacity, width))

    def rows_first(array):
        return array.transpose(1, 0, 2, 3).reshape(here, -1, array.shape[-1])

    return (
        mixed,
        rows_first(gate_up_new[..., :hidden_width]),
        rows_first(gate_up_new[..., hidden_width:]),
        rows_first(down_new),
    )


def solution(mesh):
    in_specs = (
        P("fs", None),
        P("fs", None),
        P("fs", None),
        P("fs"),
        P(None, "fs", "tp"),
        P(None, "fs", "tp"),
        P(None, "fs", "tp"),
    )
    out_specs = (P("fs", "tp"), P("fs", None, "tp"), P("fs", None, "tp"), P("fs", None, "tp"))
    return jax.shard_map(layer, mesh=mesh, in_specs=in_specs, out_specs=out_specs, check_vma=False)
```

```python
import functools
import jax
import jax.numpy as jnp
from jax import lax
from jax.experimental import pallas as pl
from jax.experimental.pallas import tpu as pltpu
from jax.sharding import PartitionSpec as P

norm_eps = 1e-06
MIB = 1024 * 1024


def dispatch_kernel(cap, tp_ref, routes_ref, prompt_ref, out_ref, slots_ref, held, normed, key, choice, outbox, in_sem, out_sem):
    parts, rows, _ = held.shape
    experts, tokens = key.shape
    width = normed.shape[1]
    block = outbox.shape[1]
    loads = [
        pltpu.make_async_copy(prompt_ref.at[pl.ds(k * rows, rows)], held.at[k], in_sem.at[k])
        for k in range(parts)
    ]
    for load in loads:
        load.start()

    ids = routes_ref[...]
    expert = lax.broadcasted_iota(jnp.int32, (experts, tokens), 0)
    hit0 = ids[0:1, :] == expert
    hit1 = ids[1:2, :] == expert
    named = hit0 | hit1
    earlier = lax.broadcasted_iota(jnp.int32, (tokens, tokens), 0) < lax.broadcasted_iota(
        jnp.int32, (tokens, tokens), 1
    )
    count = jnp.dot(
        jnp.where(named, 1.0, 0.0).astype(jnp.bfloat16),
        jnp.where(earlier, 1.0, 0.0).astype(jnp.bfloat16),
        preferred_element_type=jnp.float32,
    )
    key[...] = jnp.where(named, count, -1.0).astype(jnp.int32)
    rank0 = jnp.sum(jnp.where(hit0, count, 0.0), axis=0, keepdims=True).astype(jnp.int32)
    rank1 = jnp.sum(jnp.where(hit1, count, 0.0), axis=0, keepdims=True).astype(jnp.int32)
    slots_ref[0:1, :] = ids[0:1, :] * cap + rank0
    slots_ref[1:2, :] = ids[1:2, :] * cap + rank1

    def fill(group, _):
        rank = lax.broadcasted_iota(jnp.int32, (cap, tokens), 0)
        first = pl.multiple_of(group * 8, 8)
        keys = key[pl.ds(first, 8), :]
        for k in range(8):
            choice[pl.ds(pl.multiple_of((first + k) * cap, cap), cap), :] = jnp.where(
                keys[k : k + 1, :] == rank, 1.0, 0.0
            ).astype(jnp.bfloat16)
        return 0

    lax.fori_loop(0, experts // 8, fill, 0)

    start = pl.multiple_of(tp_ref[0] * width, width)
    for k in range(parts):
        loads[k].wait()
        values = held[k].astype(jnp.float32)
        scale = lax.rsqrt(jnp.mean(values * values, axis=1, keepdims=True) + norm_eps)
        part = held[k, :, pl.ds(start, width)].astype(jnp.float32)
        normed[pl.ds(k * rows, rows), :] = (part * scale).astype(jnp.bfloat16)

    stores = []
    for k in range(outbox.shape[0]):
        outbox[k] = jnp.dot(
            choice[pl.ds(k * block, block), :], normed[...], preferred_element_type=jnp.float32
        ).astype(jnp.bfloat16)
        stores.append(
            pltpu.make_async_copy(outbox.at[k], out_ref.at[pl.ds(k * block, block)], out_sem.at[k])
        )
        stores[k].start()
    for store in stores:
        store.wait()


def dispatch(prompt, routes, tp_index, cap, experts, width):
    tokens, model_width = prompt.shape
    parts = 2
    rows, block = tokens // parts, experts * cap // parts
    return pl.pallas_call(
        functools.partial(dispatch_kernel, cap),
        in_specs=[
            pl.BlockSpec(memory_space=pltpu.SMEM),
            pl.BlockSpec(memory_space=pltpu.VMEM),
            pl.BlockSpec(memory_space=pltpu.HBM),
        ],
        out_specs=[
            pl.BlockSpec(memory_space=pltpu.HBM),
            pl.BlockSpec(memory_space=pltpu.VMEM),
        ],
        scratch_shapes=[
            pltpu.VMEM((parts, rows, model_width), jnp.bfloat16),
            pltpu.VMEM((tokens, width), jnp.bfloat16),
            pltpu.VMEM((experts, tokens), jnp.int32),
            pltpu.VMEM((experts * cap, tokens), jnp.bfloat16),
            pltpu.VMEM((parts, block, width), jnp.bfloat16),
            pltpu.SemaphoreType.DMA((parts,)),
            pltpu.SemaphoreType.DMA((parts,)),
        ],
        out_shape=[
            pltpu.HBM((experts * cap, width), jnp.bfloat16),
            jax.ShapeDtypeStruct((2, tokens), jnp.int32),
        ],
        compiler_params=pltpu.CompilerParams(vmem_limit_bytes=48 * MIB),
        name="dispatch",
    )(tp_index, routes.T, pltpu.with_memory_space_constraint(prompt, pltpu.HBM))


def combine_kernel(slots_ref, share_ref, rows_ref, out_ref):
    tokens = slots_ref.shape[1]
    block = rows_ref.shape[0] // 12
    share = share_ref[...]
    total = None
    for k in range(12):
        slot = lax.broadcasted_iota(jnp.int32, (block, tokens), 0) + k * block
        second = jnp.where(slots_ref[1:2, :] == slot, share[1:2, :], 0.0)
        weights = jnp.where(slots_ref[0:1, :] == slot, share[0:1, :], second).astype(jnp.bfloat16)
        product = lax.dot_general(
            weights,
            rows_ref[pl.ds(k * block, block), :],
            (((0,), (0,)), ((), ())),
            preferred_element_type=jnp.float32,
        )
        total = product if total is None else total + product
    out_ref[...] = total.astype(jnp.bfloat16)


def combine(slots, share, rows):
    whole = pl.BlockSpec(memory_space=pltpu.VMEM)
    return pl.pallas_call(
        combine_kernel,
        in_specs=[whole] * 3,
        out_specs=whole,
        out_shape=jax.ShapeDtypeStruct((slots.shape[1], rows.shape[1]), jnp.bfloat16),
        compiler_params=pltpu.CompilerParams(vmem_limit_bytes=48 * MIB),
        name="combine",
    )(slots, share, rows)


PLACES = ((0, 0), (0, 1), (3, 0), (3, 1), (1, 0), (1, 1), (2, 0), (2, 1))


def expert_matmul_kernel(gated, blocks, begin, out_begin, tp_ref, *refs):
    pieces, weight_ref, out_ref = refs[:8], refs[8], refs[-7]
    held, matrices, result, piece_sem, weight_sem, out_sem = refs[-6:]
    experts, count, cap, _ = held.shape
    width = pieces[0].shape[-1]
    index = tp_ref[0]

    weight_loads = [
        pltpu.make_async_copy(weight_ref.at[:, e], matrices.at[e], weight_sem.at[e])
        for e in range(experts)
    ]
    loads = []
    for p in range(8):
        dx, swap = PLACES[p]
        source = (((index >> 1) + dx) & 3) * 2 + ((index & 1) ^ swap)
        first = begin if pieces[p].shape[0] > count else 0
        loads.append(
            [
                pltpu.make_async_copy(
                    pieces[p].at[pl.ds(first, count), e],
                    held.at[e, :, :, pl.ds(pl.multiple_of(source * width, width), width)],
                    piece_sem.at[e, p],
                )
                for e in range(experts)
            ]
        )
    for e in range(experts):
        weight_loads[e].start()
        for p in range(8):
            loads[p][e].start()

    stores = []
    part = count // blocks
    for e in range(experts):
        weight_loads[e].wait()
        for p in range(8):
            loads[p][e].wait()
        right = matrices[e].reshape(8 * width, matrices.shape[-1])
        for b in range(blocks):
            span = pl.ds(b * part, part)
            left = held[e, span].reshape(part * cap, 8 * width)
            total = jnp.dot(left, right, preferred_element_type=jnp.float32)
            if gated:
                half = total.shape[1] // 2
                gate, up = total[:, :half], total[:, half:]
                total = gate / (1.0 + jnp.exp(-gate)) * up
            result[e, span] = total.astype(jnp.bfloat16).reshape((part,) + result.shape[2:])
        stores.append(
            pltpu.make_async_copy(
                result.at[e], out_ref.at[pl.ds(out_begin, count), e], out_sem.at[e]
            )
        )
        stores[e].start()
    for store in stores:
        store.wait()


def expert_matmul(pieces, weight, tp_index, half, gated, blocks, into):
    cap, width = pieces[0].shape[-2:]
    sources, experts = weight.shape[0], weight.shape[1]
    out_width = weight.shape[-1] // 2 if gated else weight.shape[-1]
    count = sources // 2
    anywhere = pl.BlockSpec(memory_space=pl.ANY)
    operands = [*pieces, weight]
    aliases = {}
    if into is not None:
        operands.append(into)
        aliases = {len(operands): 0}
    out_shape = pltpu.HBM((count if gated else sources, experts, cap, out_width), jnp.bfloat16)
    operands = [pltpu.with_memory_space_constraint(array, pltpu.HBM) for array in operands]
    return pl.pallas_call(
        functools.partial(
            expert_matmul_kernel, gated, blocks, half * count, 0 if gated else half * count
        ),
        in_specs=[pl.BlockSpec(memory_space=pltpu.SMEM)] + [anywhere] * len(operands),
        out_specs=pl.BlockSpec(memory_space=pltpu.HBM),
        out_shape=out_shape,
        scratch_shapes=[
            pltpu.VMEM((experts, count, cap, 8 * width), jnp.bfloat16),
            pltpu.VMEM((experts, sources) + weight.shape[2:], jnp.bfloat16),
            pltpu.VMEM((experts, count, cap, out_width), jnp.bfloat16),
            pltpu.SemaphoreType.DMA((experts, 8)),
            pltpu.SemaphoreType.DMA((experts,)),
            pltpu.SemaphoreType.DMA((experts,)),
        ],
        input_output_aliases=aliases,
        compiler_params=pltpu.CompilerParams(vmem_limit_bytes=48 * MIB),
    )(tp_index, *operands)


def tp_move(dx, swap):
    return [(2 * x + c, 2 * ((x + dx) % 4) + (c ^ swap)) for x in range(4) for c in range(2)]


def move(array, dx, swap):
    return lax.ppermute(array, "tp", tp_move(dx, swap))


def spread_tokens(own):
    half = own.shape[0] // 2
    first, second = own[:half], own[half:]
    right_first = move(first, 1, 0)
    left_second = move(second, 3, 0)
    right_second = move(second, 1, 0)
    left_first = move(first, 3, 0)
    own_other = move(own, 0, 1)
    far_first = move(right_first, 1, 0)
    far_second = move(left_second, 3, 0)

    def both(piece):
        return piece, move(piece, 0, 1)

    return (
        (own, own_other)
        + both(right_first)
        + both(left_first)
        + both(far_first),
        (own, own_other)
        + both(right_second)
        + both(left_second)
        + both(far_second),
    )


def spread_hidden(own, half):
    right = move(own, 1, 0)
    left = move(own, 3, 0)
    far = move(right, 1, 0) if half == 0 else move(left, 3, 0)
    own_other = move(own, 0, 1)
    right_other = move(right, 0, 1)
    left_other = move(left, 0, 1)
    far_other = move(far, 0, 1)
    return own, own_other, right, right_other, left, left_other, far, far_other


def exchange(array):
    return lax.all_to_all(array, "fs", split_axis=0, concat_axis=0, tiled=True)


def layer(prompt, routes, affinity, norm_gain, gate_master, up_master, down_master):
    fs_count, tp_count = lax.axis_size("fs"), lax.axis_size("tp")
    experts, gain_rows, hidden_width = gate_master.shape
    here = experts // fs_count
    token_count, top_count = routes.shape
    capacity = 2 * token_count * top_count // experts
    width = prompt.shape[1] // tp_count
    tp_index = lax.axis_index("tp").astype(jnp.int32)
    tp_index = tp_index.reshape(1)

    outbox, slots = dispatch(prompt, routes, tp_index, capacity, experts, width)
    received = exchange(outbox.reshape(fs_count, here, capacity, width))

    gain = norm_gain[None, :, None]
    gate_up = jnp.concatenate(
        [(gate_master * gain).astype(jnp.bfloat16), (up_master * gain).astype(jnp.bfloat16)], axis=2
    ).reshape(fs_count, here, gain_rows, 2 * hidden_width)
    pieces = spread_tokens(received)
    swapped = [piece for half in pieces for piece in half[1::2]]
    affinity = lax.optimization_barrier((affinity, *swapped))[0].T
    share = affinity / jnp.sum(affinity, axis=0, keepdims=True)
    down = down_master.astype(jnp.bfloat16)
    down = down.reshape((fs_count, here) + down_master.shape[1:])
    gate_up_new = exchange(gate_up)
    down_new = exchange(down)
    hidden = [
        spread_hidden(expert_matmul(pieces[half], gate_up_new, tp_index, half, True, 2, None), half)
        for half in range(2)
    ]
    expert_out = None
    for half in range(2):
        expert_out = expert_matmul(hidden[half], down_new, tp_index, half, False, 2, expert_out)
    returned = exchange(expert_out)
    mixed = combine(slots, share, returned.reshape(experts * capacity, width))

    def rows_first(array):
        return array.transpose(1, 0, 2, 3).reshape(here, -1, array.shape[-1])

    return (
        mixed,
        rows_first(gate_up_new[..., :hidden_width]),
        rows_first(gate_up_new[..., hidden_width:]),
        rows_first(down_new),
    )


def solution(mesh):
    in_specs = (
        P("fs", None),
        P("fs", None),
        P("fs", None),
        P("fs"),
        P(None, "fs", "tp"),
        P(None, "fs", "tp"),
        P(None, "fs", "tp"),
    )
    out_specs = (P("fs", "tp"), P("fs", None, "tp"), P("fs", None, "tp"), P("fs", None, "tp"))
    return jax.shard_map(layer, mesh=mesh, in_specs=in_specs, out_specs=out_specs, check_vma=False)
```
